32 devices in a mesh: sp: 16 (over z, y, x), tp: 2 (over core).
Axes of the slice: x: 2, y: 2, z: 4, core: 2. Of those that a mesh axis runs over, the one named last changes fastest.
Arguments:
- residual: bfloat16 [4096, 2048], P(('sp', 'tp')), may hold values from -6 to 6
- query_one: bfloat16 [4096, 512], P('sp', 'tp'), may hold values from -6.5 to 6.5
- key_one: bfloat16 [4096, 512], P('sp', 'tp'), may hold values from -6.5 to 6.5
- query_two: bfloat16 [4096, 512], P('sp', 'tp'), may hold values from -6.5 to 6.5
- key_two: bfloat16 [4096, 512], P('sp', 'tp'), may hold values from -6.5 to 6.5
- value_rows: bfloat16 [4096, 1024], P('sp', 'tp'), may hold values from -6 to 6
- lambda_head: float32 [8], P('tp'), may hold values from 0.3 to 0.8
- head_gain: float32 [128], replicated, may hold values from 0.1 to 1.9
- out_weight: bfloat16 [1024, 2048], replicated, may hold values from -0.1875 to 0.1875
- norm_gain: float32 [2048], replicated, may hold values from 0.1 to 1.9
- route_ids: int32 [4096, 2], P(('sp', 'tp')), may hold values from 0 to 15, all different within a row; in each aligned block of 128 rows (0 to 127, 128 to 255, ...) at most 24 rows name the same one
- route_weights: float32 [4096, 2], P(('sp', 'tp')), may hold values from 0.25 to 1
- gate_weight: bfloat16 [16, 2048, 512], P('sp', None, 'tp'), may hold values from -0.125 to 0.125
- up_weight: bfloat16 [16, 2048, 512], P('sp', None, 'tp'), may hold values from -0.125 to 0.125
- down_weight: bfloat16 [16, 512, 2048], P('sp', 'tp'), may hold values from -0.25 to 0.25
Outputs:
- mixed: bfloat16 [4096, 2048], P(('sp', 'tp'))
The draws below stay inside these ranges and needn't reach their ends.
Inputs may be any that keep to these rules, and one draw needn't show every extreme that they name: `route_ids`: each row names 2 different experts. Among the rows of one device (aligned blocks of 128 rows) no expert is named more than 24 times, and in every draw some device has an expert named exactly 24 times.
All inputs are finite; a program needn't handle non-finite values.
Results may differ from the reference program's by a relative error of at most 0.014.
Values may be sent and summed in bfloat16 or wider, within the bound.
No kernel may reach another device: no remote copies, remote signals or barrier semaphores. Data moves between devices by JAX's collectives and lax.ppermute only.
A program may use at most 128 MiB of HBM per device.

```python
import math
import jax
import jax.numpy as jnp
import numpy as np
from jax import lax

D = 2048
HEADS = 8
HD = 64
VD = 128
FF = 512
TOPK = 2
TOK_DEV = 256
TOKENS = 4096
EXPERTS = 16
CAP = 24
N_SP = 16
N_TP = 2


def draw_queries(key, map_index):
    sample = 1.3 * jax.random.normal(jax.random.fold_in(key, 11 + map_index), (TOKENS, HEADS * HD), jnp.float32)
    sample = jnp.clip(sample, -6.5, 6.5)
    return sample.astype(jnp.bfloat16)


def draw_keys(key, map_index):
    sample = 1.3 * jax.random.normal(jax.random.fold_in(key, 21 + map_index), (TOKENS, HEADS * HD), jnp.float32)
    sample = jnp.clip(sample, -6.5, 6.5)
    return sample.astype(jnp.bfloat16)


def draw_query_one(key, part):
    return draw_queries(key, 0)


def draw_key_one(key, part):
    return draw_keys(key, 0)


def draw_query_two(key, part):
    return draw_queries(key, 1)


def draw_key_two(key, part):
    return draw_keys(key, 1)


def levels(key, dims, shards, least, high):
    gain = 1.0
    for dim, blocks in shards:
        heights = jax.random.uniform(jax.random.fold_in(jax.random.fold_in(key, 6), dim), (blocks,), jnp.float32, least / len(shards), high / len(shards))
        gain = gain * jnp.repeat(jnp.exp(heights), dims[dim] // blocks).reshape((-1,) + (1,) * (len(dims) - 1 - dim))
    return gain


def routed_block(rng, own, number, rows, number_of, top, limit, skew):
    order = jax.random.permutation(rng, number_of)
    packed, ordinary = shares(number_of, rows * top, limit, skew, True), shares(number_of, rows * top, limit, skew, False)
    places = jnp.arange(number_of)

    def named(lengths, turn):
        used = int((lengths > 0).sum())
        fixed = max(1, used // 4)
        shifted = fixed + (places - fixed + turn * (used - fixed)) % max(1, number_of - fixed)
        return jnp.zeros((number_of,), jnp.int32).at[order[jnp.where(places < fixed, places, shifted)]].set(jnp.asarray(lengths, jnp.int32))

    lengths = jnp.where(number % 4 == 0, named(packed, number // 4), named(ordinary, number - number // 4 - 1))
    mixed = jax.random.permutation(jax.random.fold_in(own, 3), number_of)
    giver, taker = mixed[0:number_of // 2 * 2:2], mixed[1:number_of // 2 * 2:2]
    margin = jnp.minimum(lengths[giver] - 1, limit - lengths[taker]) // 2
    margin = jnp.where((giver == order[0]) | (taker == order[0]) | (lengths[taker] == 0), 0, jnp.maximum(margin, 0))
    shifted = jax.random.randint(jax.random.fold_in(own, 4), (number_of // 2,), 0, 1 << 20) % (margin + 1)
    lengths = lengths.at[giver].add(-shifted).at[taker].add(shifted)
    members = jnp.searchsorted(jnp.cumsum(lengths), jnp.arange(rows * top), side="right").astype(jnp.int32)
    grid = members.reshape(top, rows).T
    grid = grid[jax.random.permutation(jax.random.fold_in(own, 1), rows)]
    turn = jax.random.randint(jax.random.fold_in(own, 2), (rows, 1), 0, top)
    return jnp.take_along_axis(grid, (jnp.arange(top)[None, :] + turn) % top, axis=1)


def shares(amount, total, bound, lean, full):
    loads = [(1 << 20) // math.isqrt(standing ** lean) + 1 for standing in range(1, amount + 1)]
    largest = bound if full else min(bound, max(-(-total // amount), total * loads[0] // sum(loads)))
    least = 1 if total - largest >= amount - 1 else 0
    holding, spare = [largest] + [least] * (amount - 1), total - largest - least * (amount - 1)
    while spare > 0:
        candidates = [i for i in range(1, amount) if holding[i] < largest] or [i for i in range(1, amount) if holding[i] < bound]
        whole, budget = sum([loads[i] for i in candidates]), spare
        for i in candidates:
            more = min(bound - holding[i], max(1, budget * loads[i] // whole), spare)
            holding[i] = holding[i] + more
            spare = spare - more
    return np.array(holding)


def normal_values(own_key, dims, width, most, pieces=(), kind=jnp.bfloat16):
    level = levels(own_key, dims, pieces, -0.22, 0.18) if pieces else 1.0
    values = jax.random.normal(own_key, dims, jnp.float32) * width * level
    return jnp.minimum(jnp.maximum(values, -most), most).astype(kind)


def setup_inputs(seed: int = 0) -> dict:
    seeds = jax.random.split(jax.random.key(seed), 16)
    residual = normal_values(seeds[0], (TOKENS, D), 1.0, 6.0, ((0, 32),))
    query_one = draw_query_one(jax.random.fold_in(seeds[15], 71), 0)
    key_one = draw_key_one(jax.random.fold_in(seeds[15], 71), 0)
    query_two = draw_query_two(jax.random.fold_in(seeds[15], 71), 0)
    key_two = draw_key_two(jax.random.fold_in(seeds[15], 71), 0)
    value_rows = normal_values(seeds[5], (TOKENS, HEADS * VD), 1.0, 6.0, ((0, 16), (1, 2)))
    lambda_head = jnp.clip(0.3 + 0.5 * jax.random.uniform(seeds[6], (HEADS,), jnp.float32) ** levels(seeds[6], (HEADS,), ((0, 2),), -0.2, 0.2), 0.3, 0.8)
    head_gain = jnp.clip(1.0 + 0.18 * jax.random.normal(seeds[7], (VD,), jnp.float32), 0.1, 1.9)
    out_weight = normal_values(seeds[8], (HEADS * VD, D), (HEADS * VD) ** -0.5, 0.1875)
    norm_gain = jnp.clip(1.0 + 0.18 * jax.random.normal(seeds[9], (D,), jnp.float32), 0.1, 1.9)
    route_ids_keys = jax.random.split(jax.random.fold_in(seeds[10], 1), TOKENS // (TOK_DEV // N_TP))
    route_ids_turns = jax.random.permutation(jax.random.fold_in(seeds[10], 3), TOKENS // (TOK_DEV // N_TP))
    route_ids = jax.vmap(lambda own, number: routed_block(jax.random.fold_in(seeds[10], 2), own, number, TOK_DEV // N_TP, EXPERTS, TOPK, CAP, 2))(route_ids_keys, route_ids_turns).reshape((TOKENS, TOPK))
    route_weights = jnp.clip(0.25 + 0.75 * jax.random.uniform(seeds[11], (TOKENS, TOPK), jnp.float32) ** levels(seeds[11], (TOKENS, TOPK), ((0, 32),), -0.2, 0.2), 0.25, 1.0)
    gate_weight = normal_values(seeds[12], (EXPERTS, D, FF), D ** -0.5, 0.125, ((0, 16), (2, 2)))
    up_weight = normal_values(seeds[13], (EXPERTS, D, FF), D ** -0.5, 0.125, ((0, 16), (2, 2)))
    down_weight = normal_values(seeds[14], (EXPERTS, FF, D), FF ** -0.5, 0.25, ((0, 16), (1, 2)))
    return dict(residual=residual, query_one=query_one, key_one=key_one, query_two=query_two, key_two=key_two, value_rows=value_rows, lambda_head=lambda_head, head_gain=head_gain, out_weight=out_weight, norm_gain=norm_gain, route_ids=route_ids, route_weights=route_weights, gate_weight=gate_weight, up_weight=up_weight, down_weight=down_weight)


epsilon = 1e-06

def settle(values):
    return lax.optimization_barrier(values.astype(jnp.bfloat16)).astype(jnp.float32)

def head_map(inputs, allowed):
    queries, keys, value_part = inputs
    scores = jnp.dot(queries, keys.T) * HD ** (-0.5)
    scores = jnp.where(allowed, scores, -jnp.inf)
    highest = lax.optimization_barrier(jnp.max(scores, axis=-1, keepdims=True))
    exp_weights = jnp.where(allowed, jnp.exp(scores - highest), 0.0)
    row_total = lax.optimization_barrier(jnp.sum(exp_weights, axis=-1, keepdims=True))
    summed = jnp.dot(settle(exp_weights), value_part)
    return summed / row_total

def one_map(queries, keys, value_part, allowed):
    head_queries = jnp.transpose(queries, (1, 0, 2))
    head_keys = jnp.transpose(keys, (1, 0, 2))
    head_values = jnp.transpose(value_part, (1, 0, 2))
    result = lax.map(lambda inputs: head_map(inputs, allowed), (head_queries, head_keys, head_values))
    return jnp.transpose(result, (1, 0, 2))

def attention(query_one, key_one, query_two, key_two, value_rows, lambda_head, head_gain):
    first_query = query_one.astype(jnp.float32).reshape(TOKENS, HEADS, HD)
    first_key = key_one.astype(jnp.float32).reshape(TOKENS, HEADS, HD)
    second_query = query_two.astype(jnp.float32).reshape(TOKENS, HEADS, HD)
    second_key = key_two.astype(jnp.float32).reshape(TOKENS, HEADS, HD)
    value_part = value_rows.astype(jnp.float32).reshape(TOKENS, HEADS, VD)
    outputs = []
    for segment in range(N_SP):
        begin_row = segment * TOK_DEV
        end_row = begin_row + TOK_DEV
        allowed = (begin_row + jnp.arange(TOK_DEV))[:, None] >= jnp.arange(end_row)[None, :]
        first_out = one_map(first_query[begin_row:end_row], first_key[:end_row], value_part[:end_row], allowed)
        second_out = one_map(second_query[begin_row:end_row], second_key[:end_row], value_part[:end_row], allowed)
        head_out = first_out - lambda_head[None, :, None] * second_out
        normed = head_out * lax.rsqrt(lax.optimization_barrier(jnp.mean(head_out * head_out, axis=-1, keepdims=True)) + epsilon) * head_gain
        outputs.append(normed.reshape(TOK_DEV, HEADS * VD).astype(jnp.bfloat16))
    return jnp.concatenate(outputs, axis=0)

def experts(routed, route_ids, route_weights, gate_weight, up_weight, down_weight):
    flat_ids = route_ids.reshape(-1).astype(jnp.int32)
    flat_weights = route_weights.reshape(-1)
    most_rows = N_SP * N_TP * CAP
    group_width = FF // N_TP

    def expert_step(totals, inputs):
        index, gate_one, up_one, down_one = inputs
        hits = flat_ids == index
        picked = jnp.nonzero(hits, size=most_rows, fill_value=0)[0].astype(jnp.int32)
        valid = jnp.arange(most_rows) < jnp.sum(hits.astype(jnp.int32))
        token_rows = picked // TOPK
        input_rows = routed[token_rows]
        gate = jnp.dot(input_rows, gate_one, preferred_element_type=jnp.float32)
        upper = jnp.dot(input_rows, up_one, preferred_element_type=jnp.float32)
        hidden = (jax.nn.silu(gate) * upper).astype(jnp.bfloat16)
        summed = jnp.zeros((most_rows, D), jnp.float32)
        for group in range(N_TP):
            begin_col = group * group_width
            partial_value = jnp.dot(hidden[:, begin_col:begin_col + group_width], down_one[begin_col:begin_col + group_width], preferred_element_type=jnp.float32)
            summed = summed + settle(partial_value)
        result = settle(summed)
        weight = jnp.where(valid, flat_weights[picked], 0.0)
        totals = totals.at[token_rows].add(weight[:, None] * result)
        return (totals, None)
    steps_in = (jnp.arange(EXPERTS, dtype=jnp.int32), gate_weight, up_weight, down_weight)
    return lax.scan(expert_step, jnp.zeros((TOKENS, D), jnp.float32), steps_in)[0]

def reference(residual, query_one, key_one, query_two, key_two, value_rows, lambda_head, head_gain, out_weight, norm_gain, route_ids, route_weights, gate_weight, up_weight, down_weight):
    attended = attention(query_one, key_one, query_two, key_two, value_rows, lambda_head, head_gain)
    after = (residual.astype(jnp.float32) + jnp.dot(attended, out_weight, preferred_element_type=jnp.float32)).astype(jnp.bfloat16)
    after_float = after.astype(jnp.float32)
    routed = (after_float * lax.rsqrt(lax.optimization_barrier(jnp.mean(after_float * after_float, axis=-1, keepdims=True)) + epsilon) * norm_gain).astype(jnp.bfloat16)
    moe_out = experts(routed, route_ids, route_weights, gate_weight, up_weight, down_weight)
    return (after_float + moe_out).astype(jnp.bfloat16)
```

```python
import functools
import math

import jax
import jax.numpy as jnp
from jax import lax
from jax.experimental import pallas as pl
from jax.experimental.pallas import tpu as pltpu
from jax.sharding import PartitionSpec as P

epsilon = 1e-06
low_value = -1e30
AXES = ("sp", "tp")


class Plan:
    def __init__(self, sp_count, tp_count, local_heads):
        self.sp, self.tp, self.local = sp_count, tp_count, local_heads
        self.heads = local_heads * tp_count
        self.ranks = sp_count // self.heads
        self.rounds = [(lam, tau) for lam in range(local_heads) for tau in range(tp_count)]

    def pairs(self, target):
        found = []
        for s in range(self.sp):
            for t in range(self.tp):
                to_s, to_t = target(s // self.ranks, s % self.ranks, t)
                found.append((s * self.tp + t, to_s * self.tp + to_t))
        return found

    def spread(self, lam, tau):
        def target(group, rank, t):
            head = self.local * t + (group + lam) % self.local
            return head * self.ranks + rank, (group // self.local + tau) % self.tp

        return self.pairs(target)

    def across(self, step):
        return self.pairs(lambda group, rank, t: (group * self.ranks + (rank + step) % self.ranks, t))

    def sibling(self, step):
        return self.pairs(lambda group, rank, t: (group * self.ranks + rank, (t + step) % self.tp))


def pack_kernel(plan, head_dim, value_dim, half, group_ref, q1, k1, q2, k2, v, *outs):
    group = group_ref[0]
    for index, (lam, tau) in enumerate(plan.rounds):
        part = (group // plan.local + tau) % plan.tp
        rows = pl.ds(pl.multiple_of(part * half, half), half)
        head = (group + lam) % plan.local
        for local in range(plan.local):
            cols = slice(local * head_dim, (local + 1) * head_dim)

            @pl.when(head == local)
            def _():
                outs[index][...] = jnp.concatenate(
                    [
                        q1[rows, cols],
                        q2[rows, cols],
                        k1[rows, cols],
                        k2[rows, cols],
                        v[rows, local * value_dim : (local + 1) * value_dim],
                    ],
                    axis=1,
                )


def pack(plan, head_dim, value_dim, half, group, q1, k1, q2, k2, v):
    width = 4 * head_dim + value_dim
    vmem = pl.BlockSpec(memory_space=pltpu.VMEM)
    return pl.pallas_call(
        functools.partial(pack_kernel, plan, head_dim, value_dim, half),
        out_shape=[jax.ShapeDtypeStruct((half, width), q1.dtype)] * len(plan.rounds),
        in_specs=[pl.BlockSpec(memory_space=pltpu.SMEM)] + [vmem] * 5,
        out_specs=[vmem] * len(plan.rounds),
        name="pack",
    )(group[None], q1, k1, q2, k2, v)


def steps(number, size, body, carried):
    if number <= 8:
        for index in range(number):
            carried = body(index * size, carried)
        return carried
    return lax.fori_loop(0, number, lambda index, value: body(pl.multiple_of(index * size, size), value), carried)


def attention_kernel(plan, head_dim, value_dim, rows, chunk, tables, lam_ref, gain_ref, *refs):
    half = rows // plan.tp
    count = len(plan.rounds)
    part_count = plan.ranks * plan.tp
    q_refs = refs[:count]
    part_refs = refs[count : count + part_count]
    out_ref = refs[count + part_count]
    kv, scores = refs[count + part_count + 1 :]
    key_width = 2 * head_dim
    for part in range(part_count):
        for index in range(count):
            position = tables[1 + part * count + index]
            kv[pl.ds(pl.multiple_of(position * half, half), half), :] = part_refs[part][index]
    lane = lax.broadcasted_iota(jnp.int32, (half, key_width), 1)
    local_query = tables[0] + lax.broadcasted_iota(jnp.int32, (2, half, chunk), 1).reshape(2 * half, chunk)
    local_key = lax.broadcasted_iota(jnp.int32, (2 * half, chunk), 1)
    factor = head_dim ** (-0.5) * math.log2(math.e)
    lam = lam_ref[0]
    group_span = plan.ranks * rows
    for tile in range(count):
        query = q_refs[tile][...]
        zero = jnp.zeros_like(query)
        both = jnp.concatenate(
            [jnp.where(lane < head_dim, query, zero), jnp.where(lane >= head_dim, query, zero)], axis=0
        )
        span = (tile + 1) * group_span
        largest = jnp.full((2 * half, 128), low_value, jnp.float32)

        def score(begin, largest, past):
            part = lax.dot_general(
                both,
                kv[pl.ds(begin, chunk), :key_width],
                (((1,), (1,)), ((), ())),
                preferred_element_type=jnp.float32,
            )
            if past is not None:
                part = jnp.where(local_key + past <= local_query, part, low_value)
            scores[:, pl.ds(begin, chunk)] = part
            for col in range(0, chunk, 128):
                largest = jnp.maximum(largest, part[:, col : col + 128])
            return largest

        largest = steps(tile * group_span // chunk, chunk, lambda begin, value: score(begin, value, None), largest)
        for past in range(0, group_span, chunk):
            largest = score(tile * group_span + past, largest, past)
        highest = jnp.max(largest, axis=1, keepdims=True)
        total = jnp.zeros((2 * half, 128), jnp.float32)
        summed = jnp.zeros((2 * half, value_dim), jnp.float32)

        def accumulate(begin, carried):
            total, summed = carried
            weights = jnp.exp2((scores[:, pl.ds(begin, chunk)] - highest) * factor)
            for col in range(0, chunk, 128):
                total = total + weights[:, col : col + 128]
            summed = summed + jnp.dot(
                weights.astype(jnp.bfloat16),
                kv[pl.ds(begin, chunk), key_width:],
                preferred_element_type=jnp.float32,
            )
            return total, summed

        total, summed = steps(span // chunk, chunk, accumulate, (total, summed))
        result = summed / jnp.sum(total, axis=1, keepdims=True)
        head_out = result[:half] - lam * result[half:]
        normed = head_out * lax.rsqrt(jnp.mean(head_out * head_out, axis=-1, keepdims=True) + epsilon)
        out_ref[tile] = (normed * gain_ref[...]).astype(out_ref.dtype)


def attend(plan, head_dim, value_dim, rows, tables, lam, gain, queries, parts):
    half = rows // plan.tp
    count = len(plan.rounds)
    total = plan.sp * rows
    vmem = pl.BlockSpec(memory_space=pltpu.VMEM)
    smem = pl.BlockSpec(memory_space=pltpu.SMEM)
    return pl.pallas_call(
        functools.partial(attention_kernel, plan, head_dim, value_dim, rows, min(512, plan.ranks * rows)),
        out_shape=jax.ShapeDtypeStruct((count, half, value_dim), jnp.bfloat16),
        in_specs=[smem, smem] + [vmem] * (1 + len(queries) + len(parts)),
        out_specs=vmem,
        scratch_shapes=[
            pltpu.VMEM((total, 2 * head_dim + value_dim), jnp.bfloat16),
            pltpu.VMEM((2 * half, total), jnp.float32),
        ],
        compiler_params=pltpu.CompilerParams(vmem_limit_bytes=60 * 1024 * 1024),
        name="attend",
    )(tables, lam, gain[None, :], *queries, *parts)


def combine_kernel(after_ref, back_ref, slot_ref, weight_ref, out_ref):
    rows, choices = slot_ref.shape
    slots = back_ref.shape[0]
    column = lax.broadcasted_iota(jnp.int32, (rows, slots), 1)
    total = after_ref[...].astype(jnp.float32)
    mixed = None
    for choice in range(choices):
        pick = (column == slot_ref[:, choice : choice + 1]).astype(jnp.bfloat16)
        term = jnp.dot(pick, back_ref[...], preferred_element_type=jnp.float32) * weight_ref[:, choice : choice + 1]
        mixed = term if mixed is None else mixed + term
    out_ref[...] = (total + mixed).astype(out_ref.dtype)


def combine(after, back, slot, weights):
    vmem = pl.BlockSpec(memory_space=pltpu.VMEM)
    return pl.pallas_call(
        combine_kernel,
        out_shape=jax.ShapeDtypeStruct(after.shape, jnp.bfloat16),
        in_specs=[vmem] * 4,
        out_specs=vmem,
        compiler_params=pltpu.CompilerParams(vmem_limit_bytes=48 * 1024 * 1024),
        name="combine",
    )(after, back, slot, weights)


def on_device(
    residual,
    query_one,
    key_one,
    query_two,
    key_two,
    value_rows,
    lambda_head,
    head_gain,
    out_weight,
    norm_gain,
    route_ids,
    route_weights,
    gate_weight,
    up_weight,
    down_weight,
):
    rows = query_one.shape[0]
    local_heads = lambda_head.shape[0]
    head_dim = query_one.shape[1] // local_heads
    value_dim = value_rows.shape[1] // local_heads
    model_width = residual.shape[1]
    sp_count = lax.axis_size("sp")
    tp_count = lax.axis_size("tp")
    plan = Plan(sp_count, tp_count, local_heads)
    half = rows // tp_count
    count = len(plan.rounds)
    s = lax.axis_index("sp")
    t = lax.axis_index("tp")
    group = s // plan.ranks
    rank = s % plan.ranks
    local = group % local_heads

    messages = pack(
        plan, head_dim, value_dim, half, group, query_one, key_one, query_two, key_two, value_rows
    )
    received = [
        lax.ppermute(message, AXES, plan.spread(lam, tau))
        for message, (lam, tau) in zip(messages, plan.rounds)
    ]
    key_width = 2 * head_dim
    own = jnp.stack([message[:, key_width:] for message in received])
    queries_all = jnp.stack([message[:, :key_width] for message in received])
    parts = []
    positions = []
    for step in range(plan.ranks):
        near = own if step == 0 else lax.ppermute(own, AXES, plan.across(step))
        for flip in range(tp_count):
            parts.append(near if flip == 0 else lax.ppermute(near, AXES, plan.sibling(flip)))
            from_rank = (rank - step) % plan.ranks
            from_t = (t - flip) % tp_count
            for lam, tau in plan.rounds:
                source = ((from_t - tau) % tp_count) * local_heads + (local - lam) % local_heads
                positions.append((source * plan.ranks + from_rank) * tp_count + from_t)
    tables = jnp.stack([rank * rows + t * half] + positions).astype(jnp.int32)
    queries = []
    for tile in range(count):
        lam = (local - tile) % local_heads
        tau = (t - tile // local_heads) % tp_count
        queries.append(lax.dynamic_index_in_dim(queries_all, lam * tp_count + tau, 0, keepdims=False))
    head_t = group // local_heads
    lam_parts = lambda_head
    for flip in range(1, tp_count):
        moved = lax.ppermute(lambda_head, AXES, plan.sibling(flip))
        lam_parts = jnp.where((t - flip) % tp_count == head_t, moved, lam_parts)
    lam_own = lax.dynamic_slice_in_dim(lam_parts, local, 1, 0)
    heads_out = attend(plan, head_dim, value_dim, rows, tables, lam_own, head_gain, queries, parts)
    groups = [[g * plan.ranks + r for g in range(plan.heads)] for r in range(plan.ranks)]
    heads_in = lax.all_to_all(
        heads_out, "sp", split_axis=0, concat_axis=0, tiled=True, axis_index_groups=groups
    )
    attended = jnp.transpose(heads_in, (1, 0, 2)).reshape(half, plan.heads * value_dim)
    projected = jnp.dot(attended, out_weight, preferred_element_type=jnp.float32)
    after = (residual.astype(jnp.float32) + projected).astype(jnp.bfloat16)
    after_float = after.astype(jnp.float32)
    routed = (
        after_float
        * lax.rsqrt(jnp.mean(after_float * after_float, axis=-1, keepdims=True) + epsilon)
        * norm_gain
    ).astype(jnp.bfloat16)

    local_rows, top_count = route_ids.shape
    expert_count = gate_weight.shape[0] * sp_count
    capacity = max(2, (3 * rows + 2 * sp_count - 1) // (2 * sp_count))
    flat_ids = route_ids.reshape(-1)
    onehot = (flat_ids[:, None] == jnp.arange(expert_count)[None, :]).astype(jnp.int32)
    rank_in = jnp.sum((jnp.cumsum(onehot, axis=0) - onehot) * onehot, axis=1)
    slot = (flat_ids * capacity + rank_in).reshape(local_rows, top_count)
    slot_index = jnp.arange(expert_count * capacity)
    choose = sum(
        (slot_index[:, None] == slot[:, choice][None, :]).astype(jnp.bfloat16) for choice in range(top_count)
    )
    outgoing = jnp.dot(choose, routed, preferred_element_type=jnp.float32).astype(jnp.bfloat16)
    outgoing = outgoing.reshape(expert_count, capacity, model_width)

    weights = [(gate_weight[0], up_weight[0], down_weight[0])]
    for flip in range(1, tp_count):
        weights.append(tuple(lax.ppermute(part, AXES, plan.sibling(flip)) for part in weights[0]))
    arrived = lax.all_to_all(outgoing, "sp", split_axis=0, concat_axis=0, tiled=True)
    flat_rows = arrived.reshape(sp_count * capacity, model_width)
    result = None
    for gate_part, up_part, down_part in weights:
        gate = jnp.dot(flat_rows, gate_part, preferred_element_type=jnp.float32)
        upper = jnp.dot(flat_rows, up_part, preferred_element_type=jnp.float32)
        hidden = (jax.nn.silu(gate) * upper).astype(jnp.bfloat16)
        term = jnp.dot(hidden, down_part, preferred_element_type=jnp.float32)
        result = term if result is None else result + term
    result = result.astype(jnp.bfloat16).reshape(sp_count, capacity, model_width)
    returned = lax.all_to_all(result, "sp", split_axis=0, concat_axis=0, tiled=True)
    return combine(after, returned.reshape(expert_count * capacity, model_width), slot, route_weights)


def solution(mesh):
    placed = (
        P(("sp", "tp"), None),
        P("sp", "tp"),
        P("sp", "tp"),
        P("sp", "tp"),
        P("sp", "tp"),
        P("sp", "tp"),
        P("tp"),
        P(),
        P(),
        P(),
        P(("sp", "tp"), None),
        P(("sp", "tp"), None),
        P("sp", None, "tp"),
        P("sp", None, "tp"),
        P("sp", "tp", None),
    )
    return jax.shard_map(
        on_device, mesh=mesh, in_specs=placed, out_specs=P(("sp", "tp"), None), check_vma=False
    )
```

```python
import functools
import math

import jax
import jax.numpy as jnp
from jax import lax
from jax.experimental import pallas as pl
from jax.experimental.pallas import tpu as pltpu
from jax.sharding import PartitionSpec as P


epsilon = 1e-06
low_value = -1e30
AXES = ("sp", "tp")

EARLY = 8
EARLY = 8


class Plan:
    def __init__(self, sp_count, tp_count, local_heads):
        self.sp, self.tp, self.local = sp_count, tp_count, local_heads
        self.heads = local_heads * tp_count
        self.ranks = sp_count // self.heads

    def pairs(self, target):
        found = []
        for s in range(self.sp):
            for t in range(self.tp):
                to_s, to_t = target(s // self.ranks, s % self.ranks, t)
                found.append((s * self.tp + t, to_s * self.tp + to_t))
        return found

    def spread(self, lam):
        def target(group, rank, t):
            head = self.local * t + (group + lam) % self.local
            return head * self.ranks + rank, group // self.local

        return self.pairs(target)

    def heads_on(self, step):
        return self.pairs(lambda group, rank, t: ((group + step) % self.heads * self.ranks + rank, t))

    def across(self, step):
        return self.pairs(lambda group, rank, t: (group * self.ranks + (rank + step) % self.ranks, t))

    def sibling(self, step):
        return self.pairs(lambda group, rank, t: (group * self.ranks + rank, (t + step) % self.tp))


def pack_kernel(plan, head_dim, value_dim, place_ref, q1, k1, q2, k2, v, *refs):
    outs = refs
    group = place_ref[0]
    for lam in range(plan.local):
        head = (group + lam) % plan.local
        for local in range(plan.local):
            cols = slice(local * head_dim, (local + 1) * head_dim)

            @pl.when(head == local)
            def _():
                outs[lam][...] = jnp.concatenate(
                    [
                        q1[:, cols],
                        q2[:, cols],
                        k1[:, cols],
                        k2[:, cols],
                        v[:, local * value_dim : (local + 1) * value_dim],
                    ],
                    axis=1,
                )


def pack(plan, head_dim, value_dim, place, q1, k1, q2, k2, v):
    width = 4 * head_dim + value_dim
    vmem = pl.BlockSpec(memory_space=pltpu.VMEM)
    return pl.pallas_call(
        functools.partial(pack_kernel, plan, head_dim, value_dim),
        out_shape=[jax.ShapeDtypeStruct((q1.shape[0], width), q1.dtype)] * plan.local,
        in_specs=[pl.BlockSpec(memory_space=pltpu.SMEM)] + [vmem] * 5,
        out_specs=[vmem] * plan.local,
        name="pack",
    )(place, q1, k1, q2, k2, v)


def steps(number, size, body, carried):
    if number <= 8:
        for index in range(number):
            carried = body(index * size, carried)
        return carried
    return lax.fori_loop(0, number, lambda index, value: body(pl.multiple_of(index * size, size), value), carried)


def attention_kernel(plan, head_dim, value_dim, rows, chunk, tables, lam_ref, gain_ref, slots_ref, *refs):
    half = rows // plan.tp
    count = plan.heads
    part_count = plan.ranks * plan.tp
    part_refs = refs[:part_count]
    send_ref, kv, scores = refs[-3:]
    late_refs = refs[part_count:-3]
    group, t = tables[1], tables[2]
    local = lax.rem(group, plan.local)
    experts, _, capacity, _ = send_ref.shape
    slot_row = lax.broadcasted_iota(jnp.int32, (experts * capacity, half), 0)

    def chosen(source):
        found = slot_row == slots_ref[source, 0:1, :]
        for choice in range(1, slots_ref.shape[1]):
            found = found | (slot_row == slots_ref[source, choice : choice + 1, :])
        return found.astype(send_ref.dtype)

    for late_ref in late_refs:
        late = jnp.dot(chosen(tables[1]), late_ref[...], preferred_element_type=jnp.float32)
        for col in range(late.shape[1] // value_dim):
            piece = late[:, col * value_dim : (col + 1) * value_dim]
            send_ref[:, count + col] = piece.reshape(experts, capacity, value_dim).astype(send_ref.dtype)
    key_width = 2 * head_dim
    for part in range(part_count):
        for lam in range(plan.local):
            block = tables[3 + part * plan.local + lam]
            cols = slice(part_refs[part].shape[2] - kv.shape[1], None)
            kv[pl.ds(pl.multiple_of(block * rows, rows), rows), :] = part_refs[part][lam, :rows, cols]
    lane = lax.broadcasted_iota(jnp.int32, (half, key_width), 1)
    local_query = tables[0] + lax.broadcasted_iota(jnp.int32, (2, half, chunk), 1).reshape(2 * half, chunk)
    local_key = lax.broadcasted_iota(jnp.int32, (2 * half, chunk), 1)
    factor = head_dim ** (-0.5) * math.log2(math.e)
    lam = lam_ref[0]
    group_span = plan.ranks * rows
    for tile in range(count):
        lam_index = lax.rem(local - tile % plan.local + plan.local, plan.local)
        query = part_refs[0][lam_index, pl.ds(pl.multiple_of(t * half, half), half), :key_width]
        for flip in range(1, plan.tp):
            moved = part_refs[flip][lam_index, pl.ds(pl.multiple_of(t * half, half), half), :key_width]
            query = jnp.where(lax.rem(t - flip + plan.tp, plan.tp) == tile // plan.local, moved, query)
        zero = jnp.zeros_like(query)
        both = jnp.concatenate(
            [jnp.where(lane < head_dim, query, zero), jnp.where(lane >= head_dim, query, zero)], axis=0
        )
        span = (tile + 1) * group_span
        largest = jnp.full((2 * half, 128), low_value, jnp.float32)

        def score(begin, largest, past):
            part = lax.dot_general(
                both,
                kv[pl.ds(begin, chunk), :key_width],
                (((1,), (1,)), ((), ())),
                preferred_element_type=jnp.float32,
            )
            if past is not None:
                part = jnp.where(local_key + past <= local_query, part, low_value)
            scores[:, pl.ds(begin, chunk)] = part
            for col in range(0, chunk, 128):
                largest = jnp.maximum(largest, part[:, col : col + 128])
            return largest

        largest = steps(tile * group_span // chunk, chunk, lambda begin, value: score(begin, value, None), largest)
        for past in range(0, group_span, chunk):
            largest = score(tile * group_span + past, largest, past)
        highest = jnp.max(largest, axis=1, keepdims=True)
        total = jnp.zeros((2 * half, 128), jnp.float32)
        summed = jnp.zeros((2 * half, value_dim), jnp.float32)

        def accumulate(begin, carried):
            total, summed = carried
            weights = jnp.exp2((scores[:, pl.ds(begin, chunk)] - highest) * factor)
            for col in range(0, chunk, 128):
                total = total + weights[:, col : col + 128]
            summed = summed + jnp.dot(
                weights.astype(jnp.bfloat16),
                kv[pl.ds(begin, chunk), key_width:],
                preferred_element_type=jnp.float32,
            )
            return total, summed

        total, summed = steps(span // chunk, chunk, accumulate, (total, summed))
        result = summed / jnp.sum(total, axis=1, keepdims=True)
        head_out = result[:half] - lam * result[half:]
        normed = head_out * lax.rsqrt(jnp.mean(head_out * head_out, axis=-1, keepdims=True) + epsilon)
        attended = (normed * gain_ref[...]).astype(send_ref.dtype)
        sent = jnp.dot(chosen(tile), attended, preferred_element_type=jnp.float32)
        send_ref[:, tile] = sent.reshape(experts, capacity, value_dim).astype(send_ref.dtype)


def attend(plan, head_dim, value_dim, rows, experts, capacity, tables, lam, gain, slots, late, parts):
    half = rows // plan.tp
    count = plan.heads
    total = plan.sp * rows
    limit = 8 * half * total + 4 * total * (2 * head_dim + value_dim) + 12 * 2**20
    vmem = pl.BlockSpec(memory_space=pltpu.VMEM)
    smem = pl.BlockSpec(memory_space=pltpu.SMEM)
    return pl.pallas_call(
        functools.partial(attention_kernel, plan, head_dim, value_dim, rows, min(512, plan.ranks * rows)),
        out_shape=jax.ShapeDtypeStruct(
            (experts, count + sum(x.shape[1] for x in late) // value_dim, capacity, value_dim), jnp.bfloat16
        ),
        in_specs=[smem, smem] + [vmem] * (2 + len(parts) + len(late)),
        out_specs=vmem,
        scratch_shapes=[
            pltpu.VMEM((total, 2 * head_dim + value_dim), jnp.bfloat16),
            pltpu.VMEM((2 * half, total), jnp.float32),
        ],
        compiler_params=pltpu.CompilerParams(vmem_limit_bytes=limit),
        name="attend",
    )(tables, lam, gain[None, :], slots, *parts, *late)


def experts_kernel(head_count, weight_count, gain_ref, *refs):
    count = 3 + 3 * weight_count
    sources, out_hbm = refs[:count], refs[count]
    buffers, out_ref, routed, stream, loads, stores = refs[count + 1 : 2 * count + 1], *refs[2 * count + 1 :]
    copies = [
        pltpu.make_async_copy(source, buffer, loads.at[index])
        for index, (source, buffer) in enumerate(zip(sources, buffers))
    ]
    for copy in copies:
        copy.start()
    arrived_ref, project_ref, early_ref = buffers[:3]
    gates, downs = buffers[3 : 3 + 2 * weight_count], buffers[3 + 2 * weight_count :]
    groups, ranks, planes, capacity, value_dim = arrived_ref.shape
    width = project_ref.shape[1]
    early_width = early_ref.shape[3] - value_dim
    size = groups * capacity
    for copy in copies[:3]:
        copy.wait()

    def flat(values):
        return values.astype(jnp.float32).reshape(size, values.shape[-1])

    for rank in range(ranks):
        rows = slice(rank * size, (rank + 1) * size)
        attended = jnp.concatenate(
            [flat(arrived_ref[head, rank, :groups]) for head in range(head_count)], axis=1
        ).astype(jnp.bfloat16)
        projected = jnp.dot(attended, project_ref[...], preferred_element_type=jnp.float32)
        before = [flat(early_ref[:, rank, :, :early_width])]
        before += [flat(arrived_ref[:, rank, plane]) for plane in range(groups, planes)]
        after = (jnp.concatenate(before, axis=1) + projected).astype(jnp.bfloat16)
        stream[rows, :] = after
        after = after.astype(jnp.float32)
        scale = lax.rsqrt(jnp.mean(after * after, axis=-1, keepdims=True) + epsilon)
        routed[rows, :] = (after * scale * gain_ref[...]).astype(routed.dtype)
    hidden = []
    for part in range(weight_count):
        for copy in copies[3 + 2 * part : 5 + 2 * part]:
            copy.wait()
        gate = jnp.dot(routed[...], gates[2 * part][...], preferred_element_type=jnp.float32)
        upper = jnp.dot(routed[...], gates[2 * part + 1][...], preferred_element_type=jnp.float32)
        hidden.append((gate * jax.nn.sigmoid(gate) * upper).astype(jnp.bfloat16))
    for copy in copies[3 + 2 * weight_count :]:
        copy.wait()
    for rank in range(ranks):
        rows = slice(rank * size, (rank + 1) * size)
        total = None
        for part, down_ref in zip(hidden, downs):
            term = jnp.dot(part[rows], down_ref[...], preferred_element_type=jnp.float32)
            total = term if total is None else total + term
        total = total.astype(jnp.bfloat16).astype(jnp.float32)
        extra = flat(early_ref[:, rank, :, early_width:])
        carried = stream[rows, :].astype(jnp.float32) + (extra[:, 0:1] + extra[:, 1:2]) * total
        total = jnp.where(extra[:, 2:3] > 0.5, carried, total)
        out_ref[rank] = total.reshape(groups, capacity, width).astype(out_ref.dtype)
        pltpu.make_async_copy(out_ref.at[rank], out_hbm.at[:, rank], stores.at[rank]).start()
    for rank in range(ranks):
        pltpu.make_async_copy(out_ref.at[rank], out_hbm.at[:, rank], stores.at[rank]).wait()


def run_experts(arrived, early, project, gain, weights):
    hbm = pl.BlockSpec(memory_space=pltpu.HBM)
    flat = [arrived, project, early]
    flat += [array for part in weights for array in part[:2]] + [part[2] for part in weights]
    groups, ranks, capacity, _ = early.shape
    width = project.shape[1]
    slots = groups * ranks * capacity
    return pl.pallas_call(
        functools.partial(experts_kernel, groups, len(weights)),
        out_shape=jax.ShapeDtypeStruct((groups, ranks, capacity, width), jnp.bfloat16),
        in_specs=[pl.BlockSpec(memory_space=pltpu.VMEM)] + [hbm] * len(flat),
        out_specs=hbm,
        scratch_shapes=[pltpu.VMEM(array.shape, array.dtype) for array in flat]
        + [
            pltpu.VMEM((ranks, groups, capacity, width), jnp.bfloat16),
            pltpu.VMEM((slots, width), jnp.bfloat16),
            pltpu.VMEM((slots, width), jnp.bfloat16),
            pltpu.SemaphoreType.DMA((len(flat),)),
            pltpu.SemaphoreType.DMA((ranks,)),
        ],
        compiler_params=pltpu.CompilerParams(vmem_limit_bytes=60 * 2**20),
        name="experts",
    )(gain[None, :], *flat)


def combine_kernel(back_ref, slot_ref, weight_ref, out_ref):
    rows, choices = slot_ref.shape
    column = lax.broadcasted_iota(jnp.int32, (rows, back_ref.shape[0]), 1)
    total = None
    for choice in range(choices):
        pick = (column == slot_ref[:, choice : choice + 1]).astype(jnp.bfloat16)
        term = jnp.dot(pick, back_ref[...], preferred_element_type=jnp.float32)
        total = term if choice == 0 else total + term * weight_ref[:, choice : choice + 1]
    out_ref[...] = total.astype(out_ref.dtype)


def combine(back, slot, weights):
    vmem = pl.BlockSpec(memory_space=pltpu.VMEM)
    return pl.pallas_call(
        combine_kernel,
        out_shape=jax.ShapeDtypeStruct((slot.shape[0], back.shape[1]), jnp.bfloat16),
        in_specs=[vmem] * 3,
        out_specs=vmem,
        compiler_params=pltpu.CompilerParams(vmem_limit_bytes=16 * 2**20),
        name="combine",
    )(back, slot, weights)


def on_device(
    residual,
    query_one,
    key_one,
    query_two,
    key_two,
    value_rows,
    lambda_head,
    head_gain,
    out_weight,
    norm_gain,
    route_ids,
    route_weights,
    gate_weight,
    up_weight,
    down_weight,
):
    rows = query_one.shape[0]
    local_heads = lambda_head.shape[0]
    head_dim = query_one.shape[1] // local_heads
    value_dim = value_rows.shape[1] // local_heads
    model_width = residual.shape[1]
    sp_count = lax.axis_size("sp")
    tp_count = lax.axis_size("tp")
    plan = Plan(sp_count, tp_count, local_heads)
    half = rows // tp_count
    s = lax.axis_index("sp")
    t = lax.axis_index("tp")
    group = s // plan.ranks
    rank = s % plan.ranks
    local = group % local_heads

    local_rows, top_count = route_ids.shape
    expert_count = gate_weight.shape[0] * sp_count
    capacity = max(2, (3 * rows + 2 * sp_count - 1) // (2 * sp_count))
    capacity = (capacity + 7) // 8 * 8
    picks = top_count * local_rows
    earlier = jnp.arange(picks)[:, None] > jnp.arange(picks)[None, :]

    def slots_of(ids):
        same = (ids[:, :, None] == ids[:, None, :]) & earlier
        found = ids * capacity + jnp.sum(same.astype(jnp.int32), axis=2)
        return found.reshape(ids.shape[0], top_count, local_rows)

    turned = route_ids.T
    slot = slots_of(turned.reshape(1, picks))[0].T
    slot_index = jnp.arange(expert_count * capacity)
    first = (slot_index[:, None] == slot[:, 0][None, :]).astype(jnp.bfloat16)
    choose = first + sum(
        (slot_index[:, None] == slot[:, choice][None, :]).astype(jnp.bfloat16) for choice in range(1, top_count)
    )

    messages = pack(
        plan, head_dim, value_dim, group[None], query_one, key_one, query_two, key_two, value_rows
    )
    received = [lax.ppermute(message, AXES, plan.spread(lam)) for lam, message in enumerate(messages)]
    key_width = 2 * head_dim
    own = jnp.stack(received)
    own_keys = own[:, :rows, key_width:]
    parts = []
    positions = []
    for step in range(plan.ranks):
        near = own
        if step > 0:
            near = lax.ppermute(own_keys, AXES, plan.across(step))
        for flip in range(tp_count):
            parts.append(near if flip == 0 else lax.ppermute(near, AXES, plan.sibling(flip)))
            for lam in range(local_heads):
                source = ((t - flip) % tp_count) * local_heads + (local - lam) % local_heads
                positions.append(source * plan.ranks + (rank - step) % plan.ranks)
    tables = jnp.stack([rank * rows + t * half, group, t] + positions).astype(jnp.int32)

    own_ids, _ = lax.optimization_barrier((turned.reshape(1, picks), messages[0]))
    both_ids = [own_ids] + [lax.ppermute(own_ids, AXES, plan.sibling(flip)) for flip in range(1, tp_count)]
    both_ids = jnp.concatenate(both_ids)[(t - jnp.arange(tp_count)) % tp_count]
    by_round = [jnp.stack([lax.ppermute(both_ids, AXES, plan.spread(lam)) for lam in range(local_heads)])]
    by_round += [lax.ppermute(by_round[0], AXES, plan.sibling(flip)) for flip in range(1, tp_count)]
    by_round = lax.dynamic_index_in_dim(jnp.stack(by_round), t, 2, keepdims=False).reshape(plan.heads, picks)
    sources = jnp.arange(plan.heads)
    round_of = ((t - sources // local_heads) % tp_count) * local_heads + (local - sources) % local_heads
    slots = slots_of(by_round[round_of])
    head_t = group // local_heads
    lam_parts = lambda_head
    for flip in range(1, tp_count):
        moved = lax.ppermute(lambda_head, AXES, plan.sibling(flip))
        lam_parts = jnp.where((t - flip) % tp_count == head_t, moved, lam_parts)
    lam_own = lax.dynamic_slice_in_dim(lam_parts, local, 1, 0)

    early_width = model_width * EARLY // 8 // value_dim * value_dim
    leading = route_weights[:, 0].astype(jnp.bfloat16)
    trailing = (route_weights[:, 0] - leading.astype(jnp.float32)).astype(jnp.bfloat16)
    marks = jnp.stack([leading, trailing, jnp.ones_like(leading)], axis=1)
    marks = jnp.pad(marks, ((0, 0), (0, value_dim - marks.shape[1])))
    own_residual, _ = lax.optimization_barrier((residual, own))
    early = jnp.concatenate(
        [
            jnp.dot(choose, own_residual[:, :early_width], preferred_element_type=jnp.float32),
            jnp.dot(first, marks, preferred_element_type=jnp.float32),
        ],
        axis=1,
    ).astype(jnp.bfloat16)
    early = early.reshape(expert_count, capacity, early_width + value_dim)
    early_rows = lax.all_to_all(early, "sp", split_axis=0, concat_axis=0, tiled=True)

    sent = attend(
        plan, head_dim, value_dim, rows, expert_count, capacity, tables, lam_own, head_gain, slots,
        [residual[:, early_width:]] if early_width < model_width else [], parts,
    )
    arrived = lax.all_to_all(sent, "sp", split_axis=0, concat_axis=0, tiled=True)
    weights = [(gate_weight[0], up_weight[0], down_weight[0])]
    for flip in range(1, tp_count):
        weights.append(tuple(lax.ppermute(part, AXES, plan.sibling(flip)) for part in weights[0]))
    result = run_experts(
        arrived.reshape(plan.heads, plan.ranks, -1, capacity, value_dim),
        early_rows.reshape(plan.heads, plan.ranks, capacity, -1),
        out_weight,
        norm_gain,
        weights,
    )
    returned = lax.all_to_all(
        result.reshape(expert_count, capacity, model_width), "sp", split_axis=0, concat_axis=0, tiled=True
    )
    return combine(returned.reshape(expert_count * capacity, model_width), slot, route_weights)


def solution(mesh):
    placed = (
        P(("sp", "tp"), None),
        P("sp", "tp"),
        P("sp", "tp"),
        P("sp", "tp"),
        P("sp", "tp"),
        P("sp", "tp"),
        P("tp"),
        P(),
        P(),
        P(),
        P(("sp", "tp"), None),
        P(("sp", "tp"), None),
        P("sp", None, "tp"),
        P("sp", None, "tp"),
        P("sp", "tp", None),
    )

    return jax.shard_map(on_device, mesh=mesh, in_specs=placed, out_specs=P(("sp", "tp"), None), check_vma=False)
```

```python
import functools
import math

import jax
import jax.numpy as jnp
from jax import lax
from jax.experimental import pallas as pl
from jax.experimental.pallas import tpu as pltpu
from jax.sharding import PartitionSpec as P


epsilon = 1e-06
low_value = -1e30
AXES = ("sp", "tp")

PARTS = 4


class Plan:
    def __init__(self, sp_count, tp_count, local_heads):
        self.sp, self.tp, self.local = sp_count, tp_count, local_heads
        self.heads = local_heads * tp_count
        self.ranks = sp_count // self.heads

    def pairs(self, target):
        found = []
        for s in range(self.sp):
            for t in range(self.tp):
                to_s, to_t = target(s // self.ranks, s % self.ranks, t)
                found.append((s * self.tp + t, to_s * self.tp + to_t))
        return found

    def spread(self, lam):
        def target(group, rank, t):
            head = self.local * t + (group + lam) % self.local
            return head * self.ranks + rank, group // self.local

        return self.pairs(target)

    def heads_on(self, step):
        return self.pairs(lambda group, rank, t: ((group + step) % self.heads * self.ranks + rank, t))

    def across(self, step):
        return self.pairs(lambda group, rank, t: (group * self.ranks + (rank + step) % self.ranks, t))

    def sibling(self, step):
        return self.pairs(lambda group, rank, t: (group * self.ranks + rank, (t + step) % self.tp))


def pack_kernel(plan, head_dim, value_dim, place_ref, q1, k1, q2, k2, v, *refs):
    outs = refs
    group = place_ref[0]
    for lam in range(plan.local):
        head = (group + lam) % plan.local
        for local in range(plan.local):
            cols = slice(local * head_dim, (local + 1) * head_dim)

            @pl.when(head == local)
            def _():
                outs[lam][...] = jnp.concatenate(
                    [
                        q1[:, cols],
                        q2[:, cols],
                        k1[:, cols],
                        k2[:, cols],
                        v[:, local * value_dim : (local + 1) * value_dim],
                    ],
                    axis=1,
                )


def pack(plan, head_dim, value_dim, place, q1, k1, q2, k2, v):
    width = 4 * head_dim + value_dim
    vmem = pl.BlockSpec(memory_space=pltpu.VMEM)
    return pl.pallas_call(
        functools.partial(pack_kernel, plan, head_dim, value_dim),
        out_shape=[jax.ShapeDtypeStruct((q1.shape[0], width), q1.dtype)] * plan.local,
        in_specs=[pl.BlockSpec(memory_space=pltpu.SMEM)] + [vmem] * 5,
        out_specs=[vmem] * plan.local,
        name="pack",
    )(place, q1, k1, q2, k2, v)


def steps(number, size, body, carried):
    if number <= 8:
        for index in range(number):
            carried = body(index * size, carried)
        return carried
    return lax.fori_loop(0, number, lambda index, value: body(pl.multiple_of(index * size, size), value), carried)


def attention_kernel(plan, head_dim, value_dim, rows, chunk, tables, lam_ref, gain_ref, slots_ref, *refs):
    half = rows // plan.tp
    count = plan.heads
    part_count = plan.ranks * plan.tp
    part_refs = refs[:part_count]
    send_ref, kv, scores = refs[-3:]
    group, t = tables[1], tables[2]
    local = lax.rem(group, plan.local)
    experts, _, capacity, _ = send_ref.shape
    slot_row = lax.broadcasted_iota(jnp.int32, (experts * capacity, half), 0)

    def chosen(source):
        found = slot_row == slots_ref[source, 0:1, :]
        for choice in range(1, slots_ref.shape[1]):
            found = found | (slot_row == slots_ref[source, choice : choice + 1, :])
        return found.astype(send_ref.dtype)

    key_width = 2 * head_dim
    for part in range(part_count):
        for lam in range(plan.local):
            block = tables[3 + part * plan.local + lam]
            cols = slice(part_refs[part].shape[2] - kv.shape[1], None)
            kv[pl.ds(pl.multiple_of(block * rows, rows), rows), :] = part_refs[part][lam, :rows, cols]
    lane = lax.broadcasted_iota(jnp.int32, (half, key_width), 1)
    local_query = tables[0] + lax.broadcasted_iota(jnp.int32, (2, half, chunk), 1).reshape(2 * half, chunk)
    local_key = lax.broadcasted_iota(jnp.int32, (2 * half, chunk), 1)
    factor = head_dim ** (-0.5) * math.log2(math.e)
    lam = lam_ref[0]
    group_span = plan.ranks * rows
    for tile in range(count):
        lam_index = lax.rem(local - tile % plan.local + plan.local, plan.local)
        query = part_refs[0][lam_index, pl.ds(pl.multiple_of(t * half, half), half), :key_width]
        for flip in range(1, plan.tp):
            moved = part_refs[flip][lam_index, pl.ds(pl.multiple_of(t * half, half), half), :key_width]
            query = jnp.where(lax.rem(t - flip + plan.tp, plan.tp) == tile // plan.local, moved, query)
        zero = jnp.zeros_like(query)
        both = jnp.concatenate(
            [jnp.where(lane < head_dim, query, zero), jnp.where(lane >= head_dim, query, zero)], axis=0
        )
        span = (tile + 1) * group_span
        largest = jnp.full((2 * half, 128), low_value, jnp.float32)

        def score(begin, largest, past):
            part = lax.dot_general(
                both,
                kv[pl.ds(begin, chunk), :key_width],
                (((1,), (1,)), ((), ())),
                preferred_element_type=jnp.float32,
            )
            if past is not None:
                part = jnp.where(local_key + past <= local_query, part, low_value)
            scores[:, pl.ds(begin, chunk)] = part
            for col in range(0, chunk, 128):
                largest = jnp.maximum(largest, part[:, col : col + 128])
            return largest

        largest = steps(tile * group_span // chunk, chunk, lambda begin, value: score(begin, value, None), largest)
        for past in range(0, group_span, chunk):
            largest = score(tile * group_span + past, largest, past)
        highest = jnp.max(largest, axis=1, keepdims=True)
        total = jnp.zeros((2 * half, 128), jnp.float32)
        summed = jnp.zeros((2 * half, value_dim), jnp.float32)

        def accumulate(begin, carried):
            total, summed = carried
            weights = jnp.exp2((scores[:, pl.ds(begin, chunk)] - highest) * factor)
            for col in range(0, chunk, 128):
                total = total + weights[:, col : col + 128]
            summed = summed + jnp.dot(
                weights.astype(jnp.bfloat16),
                kv[pl.ds(begin, chunk), key_width:],
                preferred_element_type=jnp.float32,
            )
            return total, summed

        total, summed = steps(span // chunk, chunk, accumulate, (total, summed))
        result = summed / jnp.sum(total, axis=1, keepdims=True)
        head_out = result[:half] - lam * result[half:]
        normed = head_out * lax.rsqrt(jnp.mean(head_out * head_out, axis=-1, keepdims=True) + epsilon)
        attended = (normed * gain_ref[...]).astype(send_ref.dtype)
        sent = jnp.dot(chosen(tile), attended, preferred_element_type=jnp.float32)
        send_ref[:, tile] = sent.reshape(experts, capacity, value_dim).astype(send_ref.dtype)


def attend(plan, head_dim, value_dim, rows, experts, capacity, tables, lam, gain, slots, parts):
    half = rows // plan.tp
    count = plan.heads
    total = plan.sp * rows
    limit = 8 * half * total + 4 * total * (2 * head_dim + value_dim) + 12 * 2**20
    vmem = pl.BlockSpec(memory_space=pltpu.VMEM)
    smem = pl.BlockSpec(memory_space=pltpu.SMEM)
    return pl.pallas_call(
        functools.partial(attention_kernel, plan, head_dim, value_dim, rows, min(512, plan.ranks * rows)),
        out_shape=jax.ShapeDtypeStruct((experts, count, capacity, value_dim), jnp.bfloat16),
        in_specs=[smem, smem] + [vmem] * (2 + len(parts)),
        out_specs=vmem,
        scratch_shapes=[
            pltpu.VMEM((total, 2 * head_dim + value_dim), jnp.bfloat16),
            pltpu.VMEM((2 * half, total), jnp.float32),
        ],
        compiler_params=pltpu.CompilerParams(vmem_limit_bytes=limit),
        name="attend",
    )(tables, lam, gain[None, :], slots, *parts)


def experts_kernel(early_count, weight_count, place_ref, gain_ref, *refs):
    early_hbm, refs = refs[:early_count], refs[early_count:]
    arrived_hbm, refs = refs[0], refs[1:]
    count = 1 + 3 * weight_count
    sources, refs = refs[:count], refs[count:]
    buffers, refs = refs[-5 - count : -5], refs[: -5 - count] + refs[-5:]
    outs, heads, early_ref = refs[:-7], refs[-7], refs[-6]
    out_ref, routed, stream, loads, stores = refs[-5:]
    project_ref, gates, downs = buffers[0], buffers[1 : 1 + 2 * weight_count], buffers[1 + 2 * weight_count :]
    head_count, ranks, _, capacity, _ = arrived_hbm.shape
    blocks = [(piece, row) for piece in range(early_count) for row in range(early_hbm[piece].shape[0])]
    copies = [
        pltpu.make_async_copy(source, buffer, loads.at[index])
        for index, (source, buffer) in enumerate(zip(sources, buffers))
    ]
    row_copies = []
    for block, (piece, row) in enumerate(blocks):
        place = place_ref[block]
        from_heads = arrived_hbm.at[:, lax.rem(place, ranks), place // ranks]
        first = count + 2 * block
        row_copies.append(pltpu.make_async_copy(from_heads, heads.at[:, block], loads.at[first]))
        row_copies.append(pltpu.make_async_copy(early_hbm[piece].at[row], early_ref.at[block], loads.at[first + 1]))
    width = project_ref.shape[1]
    part_width = width // PARTS
    columns = [slice(part * part_width, (part + 1) * part_width) for part in range(PARTS)]
    projects = [
        pltpu.make_async_copy(
            sources[0].at[:, cols], project_ref.at[:, cols], loads.at[count + 2 * len(blocks) + part]
        )
        for part, cols in enumerate(columns)
    ]
    for copy in row_copies[::2] + projects + row_copies[1::2] + copies[1:]:
        copy.start()
    rows = len(blocks) * capacity

    def flat(values):
        return values.astype(jnp.float32).reshape(rows, values.shape[-1])

    for copy in row_copies[::2]:
        copy.wait()
    attended = jnp.concatenate([flat(heads[head]) for head in range(head_count)], axis=1).astype(jnp.bfloat16)
    projected = []
    for copy, cols in zip(projects, columns):
        copy.wait()
        projected.append(jnp.dot(attended, project_ref[:, cols], preferred_element_type=jnp.float32))
    for copy in row_copies[1::2]:
        copy.wait()
    after = flat(early_ref[:, :, :width]) + jnp.concatenate(projected, axis=1)
    after = after.astype(jnp.bfloat16)
    stream[...] = after
    after = after.astype(jnp.float32)
    scale = lax.rsqrt(jnp.mean(after * after, axis=-1, keepdims=True) + epsilon)
    routed[...] = (after * scale * gain_ref[...]).astype(routed.dtype)
    hidden = []
    for part in range(weight_count):
        for copy in copies[1 + 2 * part : 3 + 2 * part]:
            copy.wait()
        gate = jnp.dot(routed[...], gates[2 * part][...], preferred_element_type=jnp.float32)
        upper = jnp.dot(routed[...], gates[2 * part + 1][...], preferred_element_type=jnp.float32)
        hidden.append((gate * jax.nn.sigmoid(gate) * upper).astype(jnp.bfloat16))
    for copy in copies[1 + 2 * weight_count :]:
        copy.wait()
    total = None
    for part, down_ref in zip(hidden, downs):
        term = jnp.dot(part, down_ref[...], preferred_element_type=jnp.float32)
        total = term if total is None else total + term
    total = total.astype(jnp.bfloat16).astype(jnp.float32)
    extra = flat(early_ref[:, :, width:])
    carried = stream[...].astype(jnp.float32) + (extra[:, 0:1] + extra[:, 1:2]) * total
    total = jnp.where(extra[:, 2:3] > 0.5, carried, total)
    out_ref[...] = total.reshape(out_ref.shape).astype(out_ref.dtype)
    results = []
    for block, (piece, row) in enumerate(blocks):
        results.append(pltpu.make_async_copy(out_ref.at[block], outs[piece].at[row], stores.at[block]))
    for copy in results:
        copy.start()
    for copy in results:
        copy.wait()


def run_experts(arrived, early, project, gain, weights):
    hbm = pl.BlockSpec(memory_space=pltpu.HBM)
    flat = [project]
    flat += [array for part in weights for array in part[:2]] + [part[2] for part in weights]
    head_count, _, _, capacity, value_dim = arrived.shape
    places = jnp.concatenate([place + jnp.arange(piece.shape[0]) for place, piece in early]).astype(jnp.int32)
    pieces = [piece for _, piece in early]
    width = project.shape[1]
    blocks = sum(piece.shape[0] for piece in pieces)
    rows = blocks * capacity
    return pl.pallas_call(
        functools.partial(experts_kernel, len(pieces), len(weights)),
        out_shape=[jax.ShapeDtypeStruct((piece.shape[0], capacity, width), jnp.bfloat16) for piece in pieces],
        in_specs=[pl.BlockSpec(memory_space=pltpu.SMEM), pl.BlockSpec(memory_space=pltpu.VMEM)]
        + [hbm] * (len(pieces) + 1 + len(flat)),
        out_specs=[hbm] * len(pieces),
        scratch_shapes=[
            pltpu.VMEM((head_count, blocks, capacity, value_dim), jnp.bfloat16),
            pltpu.VMEM((blocks, capacity, pieces[0].shape[2]), jnp.bfloat16),
        ]
        + [pltpu.VMEM(array.shape, array.dtype) for array in flat]
        + [
            pltpu.VMEM((blocks, capacity, width), jnp.bfloat16),
            pltpu.VMEM((rows, width), jnp.bfloat16),
            pltpu.VMEM((rows, width), jnp.bfloat16),
            pltpu.SemaphoreType.DMA((len(flat) + 2 * blocks + PARTS,)),
            pltpu.SemaphoreType.DMA((blocks,)),
        ],
        compiler_params=pltpu.CompilerParams(vmem_limit_bytes=56 * 2**20),
    )(places, gain[None, :], *pieces, arrived, *flat)


def combine_kernel(slot_ref, weight_ref, *refs):
    pieces, out_ref = refs[:-1], refs[-1]
    rows, choices = slot_ref.shape
    width = out_ref.shape[1]
    values = [ref[...].astype(jnp.float32).reshape(-1, width) for ref in pieces]
    values = jnp.concatenate(values, axis=0).astype(jnp.bfloat16)
    column = lax.broadcasted_iota(jnp.int32, (rows, values.shape[0]), 1)
    total = None
    for choice in range(choices):
        pick = (column == slot_ref[:, choice : choice + 1]).astype(jnp.bfloat16)
        term = jnp.dot(pick, values, preferred_element_type=jnp.float32)
        total = term if choice == 0 else total + term * weight_ref[:, choice : choice + 1]
    out_ref[...] = total.astype(out_ref.dtype)


def combine(pieces, slot, weights):
    vmem = pl.BlockSpec(memory_space=pltpu.VMEM)
    return pl.pallas_call(
        combine_kernel,
        out_shape=jax.ShapeDtypeStruct((slot.shape[0], pieces[0].shape[2]), jnp.bfloat16),
        in_specs=[vmem] * (2 + len(pieces)),
        out_specs=vmem,
        compiler_params=pltpu.CompilerParams(vmem_limit_bytes=24 * 2**20),
        name="combine",
    )(slot, weights, *pieces)


def exchange(values, s, sp_count):
    if sp_count & (sp_count - 1) or sp_count > 16:
        return [(jnp.int32(0), lax.all_to_all(values, "sp", split_axis=0, concat_axis=0, tiled=True))]
    side = sp_count // 2
    came = []
    for step in range(side, sp_count):
        piece = lax.dynamic_slice_in_dim(values, s ^ step, 1, 0)
        piece = lax.ppermute(piece, "sp", [(source, source ^ step) for source in range(sp_count)])
        came.append((s ^ step, piece))
    first = s // side * side
    piece = lax.dynamic_slice_in_dim(values, first, side, 0)
    sides = [list(range(begin, begin + side)) for begin in (0, side)]
    piece = lax.all_to_all(piece, "sp", split_axis=0, concat_axis=0, tiled=True, axis_index_groups=sides)
    came.append((first, piece))
    return came


def on_device(
    residual,
    query_one,
    key_one,
    query_two,
    key_two,
    value_rows,
    lambda_head,
    head_gain,
    out_weight,
    norm_gain,
    route_ids,
    route_weights,
    gate_weight,
    up_weight,
    down_weight,
):
    rows = query_one.shape[0]
    local_heads = lambda_head.shape[0]
    head_dim = query_one.shape[1] // local_heads
    value_dim = value_rows.shape[1] // local_heads
    model_width = residual.shape[1]
    sp_count = lax.axis_size("sp")
    tp_count = lax.axis_size("tp")
    plan = Plan(sp_count, tp_count, local_heads)
    half = rows // tp_count
    s = lax.axis_index("sp")
    t = lax.axis_index("tp")
    group = s // plan.ranks
    rank = s % plan.ranks
    local = group % local_heads

    local_rows, top_count = route_ids.shape
    expert_count = gate_weight.shape[0] * sp_count
    capacity = max(2, (3 * rows + 2 * sp_count - 1) // (2 * sp_count))
    capacity = (capacity + 7) // 8 * 8
    picks = top_count * local_rows
    earlier = jnp.arange(picks)[:, None] > jnp.arange(picks)[None, :]

    def slots_of(ids):
        same = (ids[:, :, None] == ids[:, None, :]) & earlier
        found = ids * capacity + jnp.sum(same.astype(jnp.int32), axis=2)
        return found.reshape(ids.shape[0], top_count, local_rows)

    turned = route_ids.T
    slot = slots_of(turned.reshape(1, picks))[0].T
    slot_index = jnp.arange(expert_count * capacity)
    first = (slot_index[:, None] == slot[:, 0][None, :]).astype(jnp.bfloat16)
    choose = first + sum(
        (slot_index[:, None] == slot[:, choice][None, :]).astype(jnp.bfloat16) for choice in range(1, top_count)
    )

    messages = pack(
        plan, head_dim, value_dim, group[None], query_one, key_one, query_two, key_two, value_rows
    )
    received = [lax.ppermute(message, AXES, plan.spread(lam)) for lam, message in enumerate(messages)]
    key_width = 2 * head_dim
    own = jnp.stack(received)
    own_keys = own[:, :rows, key_width:]
    parts = []
    positions = []
    for step in range(plan.ranks):
        near = own
        if step > 0:
            near = lax.ppermute(own_keys, AXES, plan.across(step))
        for flip in range(tp_count):
            parts.append(near if flip == 0 else lax.ppermute(near, AXES, plan.sibling(flip)))
            for lam in range(local_heads):
                source = ((t - flip) % tp_count) * local_heads + (local - lam) % local_heads
                positions.append(source * plan.ranks + (rank - step) % plan.ranks)
    tables = jnp.stack([rank * rows + t * half, group, t] + positions).astype(jnp.int32)

    own_ids, _ = lax.optimization_barrier((turned.reshape(1, picks), messages[0]))
    both_ids = [own_ids] + [lax.ppermute(own_ids, AXES, plan.sibling(flip)) for flip in range(1, tp_count)]
    both_ids = jnp.concatenate(both_ids)[(t - jnp.arange(tp_count)) % tp_count]
    by_round = [jnp.stack([lax.ppermute(both_ids, AXES, plan.spread(lam)) for lam in range(local_heads)])]
    by_round += [lax.ppermute(by_round[0], AXES, plan.sibling(flip)) for flip in range(1, tp_count)]
    by_round = lax.dynamic_index_in_dim(jnp.stack(by_round), t, 2, keepdims=False).reshape(plan.heads, picks)
    sources = jnp.arange(plan.heads)
    round_of = ((t - sources // local_heads) % tp_count) * local_heads + (local - sources) % local_heads
    slots = slots_of(by_round[round_of])
    head_t = group // local_heads
    lam_parts = lambda_head
    for flip in range(1, tp_count):
        moved = lax.ppermute(lambda_head, AXES, plan.sibling(flip))
        lam_parts = jnp.where((t - flip) % tp_count == head_t, moved, lam_parts)
    lam_own = lax.dynamic_slice_in_dim(lam_parts, local, 1, 0)

    leading = route_weights[:, 0].astype(jnp.bfloat16)
    trailing = (route_weights[:, 0] - leading.astype(jnp.float32)).astype(jnp.bfloat16)
    marks = jnp.stack([leading, trailing, jnp.ones_like(leading)], axis=1)
    marks = jnp.pad(marks, ((0, 0), (0, value_dim - marks.shape[1])))
    own_residual, _ = lax.optimization_barrier((residual, messages[0]))
    early = jnp.concatenate(
        [
            jnp.dot(choose, own_residual, preferred_element_type=jnp.float32),
            jnp.dot(first, marks, preferred_element_type=jnp.float32),
        ],
        axis=1,
    ).astype(jnp.bfloat16)
    early = early.reshape(expert_count, capacity, model_width + value_dim)
    early_rows = exchange(early, s, sp_count)

    sent = attend(
        plan, head_dim, value_dim, rows, expert_count, capacity, tables, lam_own, head_gain, slots,
        parts,
    )
    arrived = lax.all_to_all(sent, "sp", split_axis=0, concat_axis=0, tiled=True)
    weights = [(gate_weight[0], up_weight[0], down_weight[0])]
    for flip in range(1, tp_count):
        weights.append(tuple(lax.ppermute(part, AXES, plan.sibling(flip)) for part in weights[0]))
    arrived = arrived.reshape(plan.heads, plan.ranks, -1, capacity, value_dim)
    far, close = early_rows[:-1], early_rows[-1]
    returned = []
    if far:
        results = run_experts(arrived, far, out_weight, norm_gain, weights)
        for step, piece in zip(range(sp_count // 2, sp_count), results):
            pairs = [(source, source ^ step) for source in range(sp_count)]
            returned.append(lax.ppermute(piece, "sp", pairs))
    side = close[1].shape[0]
    sides = [list(range(begin, begin + side)) for begin in range(0, sp_count, side)]
    (result,) = run_experts(arrived, [close], out_weight, norm_gain, weights)
    returned.append(
        lax.all_to_all(result, "sp", split_axis=0, concat_axis=0, tiled=True, axis_index_groups=sides)
    )
    if far:
        expert, place = slot // capacity, slot % capacity
        index = jnp.where(expert // side == s // side, side + expert % side, (expert ^ s) % side)
        slot = index * capacity + place
    return combine(returned, slot, route_weights)


def solution(mesh):
    placed = (
        P(("sp", "tp"), None),
        P("sp", "tp"),
        P("sp", "tp"),
        P("sp", "tp"),
        P("sp", "tp"),
        P("sp", "tp"),
        P("tp"),
        P(),
        P(),
        P(),
        P(("sp", "tp"), None),
        P(("sp", "tp"), None),
        P("sp", None, "tp"),
        P("sp", None, "tp"),
        P("sp", "tp", None),
    )

    return jax.shard_map(on_device, mesh=mesh, in_specs=placed, out_specs=P(("sp", "tp"), None), check_vma=False)
```
